32 devices in a mesh: ep: 16 (over z, y, x), tp: 2 (over core).
Axes of the slice: x: 2, y: 2, z: 4, core: 2. Of those that a mesh axis runs over, the one named last changes fastest.
Arguments:
- tokens: bfloat16 [256, 2048], P('ep'), may hold values from -6 to 6
- norm_gain: bfloat16 [2048], replicated, may hold values from 0.099609375 to 1.8984375
- w_query: bfloat16 [2048, 512], P(None, 'tp'), may hold values from -0.125 to 0.125
- w_key: bfloat16 [2048, 256], P(None, 'tp'), may hold values from -0.125 to 0.125
- w_value: bfloat16 [2048, 256], P(None, 'tp'), may hold values from -0.125 to 0.125
- w_forget: bfloat16 [2048, 8], P(None, 'tp'), may hold values from -0.25 to 0.25
- w_out: bfloat16 [512, 2048], P('tp'), may hold values from -0.25 to 0.25
- cache_keys: bfloat16 [256, 1024, 256], P('ep', None, 'tp'), may hold values from -700 to 700
- cache_values: bfloat16 [256, 1024, 256], P('ep', None, 'tp'), may hold values from -6 to 6
- cache_gates: float32 [256, 8, 1024], P('ep', 'tp'), as said below
- lengths: int32 [256], P('ep'), may hold values from 1 to 1024, as said below
- ffn_gain: bfloat16 [2048], replicated, may hold values from 0.099609375 to 1.8984375
- router_w: bfloat16 [2048, 16], replicated, may hold values from -0.125 to 0.125
- routes: int32 [256, 6], P('ep'), may hold values from 0 to 15, all different within a row; in each aligned block of 16 rows (0 to 15, 16 to 31, ...) at most 12 rows name the same one
- shared_gate: bfloat16 [2048, 512], P(None, 'tp'), may hold values from -0.125 to 0.125
- shared_up: bfloat16 [2048, 512], P(None, 'tp'), may hold values from -0.125 to 0.125
- shared_down: bfloat16 [512, 2048], P('tp'), may hold values from -0.25 to 0.25
- expert_gate: bfloat16 [16, 2048, 512], P('ep', None, 'tp'), may hold values from -0.125 to 0.125
- expert_up: bfloat16 [16, 2048, 512], P('ep', None, 'tp'), may hold values from -0.125 to 0.125
- expert_down: bfloat16 [16, 512, 2048], P('ep', 'tp'), may hold values from -0.25 to 0.25
Outputs:
- layer_out: bfloat16 [256, 2048], P('ep')
The draws below stay inside these ranges and needn't reach their ends.
Inputs may be any that keep to these rules, and one draw needn't show every extreme that they name: `routes`: each row names 6 different experts. Among the rows of one index of ep no expert is named by more than 12 rows, and in every draw some expert is named by exactly 12 of them. `lengths`: in every draw some sequence has all 1024 positions. `cache_gates`: each row is non-increasing along the positions.
All inputs are finite; a program needn't handle non-finite values.
Results may differ from the reference program's by a relative error of at most 0.017.
Values may be sent and summed in bfloat16 or wider, within the bound.
A program may use at most 64 MiB of HBM per device.

```python
import math
import jax
import jax.numpy as jnp
import numpy as np
from jax import lax

D = 2048
QUERY_HEADS = 8
KV_HEADS = 4
HEAD_DIM = 64
SHARED_FF = 512
EXPERT_FF = 512
TOP_K = 6
SEQ_DEV = 16
CACHE_POSITIONS = 1024
SEQUENCE_TOTAL = 256
EXPERTS = 16
CAP = 12
N_EP = 16
N_TP = 2


def draw_cache_keys(key, part):
    random_split_keys = jax.random.split(jax.random.fold_in(key, 11), 1)
    base_keys = jnp.clip(jax.random.normal(random_split_keys[0], (SEQUENCE_TOTAL, CACHE_POSITIONS, KV_HEADS * HEAD_DIM), jnp.float32), -6.0, 6.0)
    return base_keys.astype(jnp.bfloat16)


def draw_cache_gates(key, part):
    random_split_keys = jax.random.split(jax.random.fold_in(key, 23), 6)
    head_order = jax.random.permutation(random_split_keys[0], QUERY_HEADS)
    slow_heads = head_order < QUERY_HEADS // 2
    block_index = jnp.arange(SEQUENCE_TOTAL) // SEQ_DEV
    processor_multiplier = jnp.exp(jax.random.uniform(random_split_keys[1], (SEQUENCE_TOTAL // SEQ_DEV,), jnp.float32, 0.0, math.log(3.0)))[block_index]
    fast_rate = 1.0 / jnp.exp(jax.random.uniform(random_split_keys[2], (QUERY_HEADS,), jnp.float32, math.log(25.0), math.log(50.0)))
    increment_speed = jnp.where(slow_heads, 0.4 / CACHE_POSITIONS, fast_rate)
    jaggedness = jax.random.uniform(random_split_keys[3], (SEQUENCE_TOTAL, QUERY_HEADS, CACHE_POSITIONS), jnp.float32, 0.3, 1.7)
    spike_position = jax.random.uniform(random_split_keys[4], (SEQUENCE_TOTAL, QUERY_HEADS, CACHE_POSITIONS)) < 2.0 / CACHE_POSITIONS
    spike_magnitude = jnp.where(spike_position, jax.random.uniform(random_split_keys[5], (SEQUENCE_TOTAL, QUERY_HEADS, CACHE_POSITIONS), jnp.float32, 0.22, 0.69), 0.0)
    logarithm_step_count = -(increment_speed[None, :, None] * processor_multiplier[:, None, None] * jaggedness + spike_magnitude)
    return jnp.cumsum(logarithm_step_count, axis=2)


def draw_lengths(key, part):
    random_split_keys = jax.random.split(jax.random.fold_in(key, 37), 3)
    block_index = jnp.arange(SEQUENCE_TOTAL) // SEQ_DEV
    shrink = jax.random.randint(random_split_keys[0], (SEQUENCE_TOTAL // SEQ_DEV,), 0, 3)
    longest = (CACHE_POSITIONS // jnp.left_shift(1, shrink))[block_index]
    drawn = jax.random.randint(random_split_keys[1], (SEQUENCE_TOTAL,), 1, longest + 1)
    full_index = jax.random.randint(random_split_keys[2], (), 0, SEQUENCE_TOTAL)
    return jnp.where(jnp.arange(SEQUENCE_TOTAL) == full_index, CACHE_POSITIONS, drawn).astype(jnp.int32)


def block_levels(own_key, dims, shards, least, high):
    def one(position, shards_of):
        heights = jax.random.uniform(jax.random.fold_in(jax.random.fold_in(own_key, 6), position), (shards_of,), jnp.float32, least / len(shards), high / len(shards))
        return jnp.repeat(jnp.exp(heights), dims[position] // shards_of).reshape((-1,) + (1,) * (len(dims) - position - 1))

    gain = one(*shards[0])
    for cut in shards[1:]:
        gain = gain * one(*cut)
    return gain


def assign_block(stream_key, own, number, rows, count, top, most, skew):
    ranking = jax.random.permutation(stream_key, count)
    heavy_load, ordinary = shares(count, rows * top, most, skew, True), shares(count, rows * top, most, skew, False)
    places = jnp.arange(count)

    def named(sizes, offset_by):
        used = int((sizes > 0).sum())
        fixed = max(1, used // 4)
        moved = fixed + (places - fixed + offset_by * (used - fixed)) % max(1, count - fixed)
        return jnp.zeros((count,), jnp.int32).at[ranking[jnp.where(places < fixed, places, moved)]].set(jnp.asarray(sizes, jnp.int32))

    sizes = jnp.where(number % 4 == 0, named(heavy_load, number // 4), named(ordinary, number - number // 4 - 1))
    mixed = jax.random.permutation(jax.random.fold_in(own, 3), count)
    source_of, receiver = mixed[0:count // 2 * 2:2], mixed[1:count // 2 * 2:2]
    slack = jnp.minimum(sizes[source_of] - 1, most - sizes[receiver]) // 2
    slack = jnp.where((source_of == ranking[0]) | (receiver == ranking[0]) | (sizes[receiver] == 0), 0, jnp.maximum(slack, 0))
    moved = jax.random.randint(jax.random.fold_in(own, 4), (count // 2,), 0, 1 << 20) % (slack + 1)
    sizes = sizes.at[source_of].add(-moved).at[receiver].add(moved)
    items = jnp.searchsorted(jnp.cumsum(sizes), jnp.arange(rows * top), side="right").astype(jnp.int32)
    grid = items.reshape(top, rows).T
    grid = grid[jax.random.permutation(jax.random.fold_in(own, 1), rows)]
    offset_by = jax.random.randint(jax.random.fold_in(own, 2), (rows, 1), 0, top)
    return jnp.take_along_axis(grid, (jnp.arange(top)[None, :] + offset_by) % top, axis=1)


def shares(count, total, limit, lean, full):
    portions = [(1 << 20) // math.isqrt(rank ** lean) + 1 for rank in range(1, count + 1)]
    largest = limit if full else min(limit, max(-(-total // count), total * portions[0] // sum(portions)))
    least = 1 if total - largest >= count - 1 else 0
    given, spare = [largest] + [least] * (count - 1), total - largest - least * (count - 1)
    while spare > 0:
        free = [i for i in range(1, count) if given[i] < largest] or [i for i in range(1, count) if given[i] < limit]
        mass, left = sum([portions[i] for i in free]), spare
        for i in free:
            more = min(limit - given[i], max(1, left * portions[i] // mass), spare)
            given[i] = given[i] + more
            spare = spare - more
    return np.array(given)


def bell_draw(key, dims, deviation, most, cuts=(), kind=jnp.bfloat16):
    values = deviation * jax.random.normal(key, dims, jnp.float32)
    if cuts:
        values = values * block_levels(key, dims, cuts, -0.22, 0.18)
    return jnp.clip(values, -most, most).astype(kind)


def setup_inputs(seed: int = 0) -> dict:
    keys = jax.random.split(jax.random.key(seed), 21)
    tokens = bell_draw(keys[0], (SEQUENCE_TOTAL, D), 1.0, 6.0, ((0, 16),))
    norm_gain = jnp.clip(1.0 + 0.18 * jax.random.normal(keys[1], (D,), jnp.float32), 0.099609375, 1.8984375).astype(jnp.bfloat16)
    w_query = bell_draw(keys[2], (D, QUERY_HEADS * HEAD_DIM), D ** -0.5, 0.125, ((1, 2),))
    w_key = bell_draw(keys[3], (D, KV_HEADS * HEAD_DIM), D ** -0.5, 0.125, ((1, 2),))
    w_value = bell_draw(keys[4], (D, KV_HEADS * HEAD_DIM), D ** -0.5, 0.125, ((1, 2),))
    w_forget = bell_draw(keys[5], (D, QUERY_HEADS), (D // 4) ** -0.5, 0.25, ((1, 2),))
    w_out = bell_draw(keys[6], (QUERY_HEADS * HEAD_DIM, D), (QUERY_HEADS * HEAD_DIM) ** -0.5, 0.25, ((0, 2),))
    cache_keys = draw_cache_keys(jax.random.fold_in(keys[20], 71), 0)
    cache_values = bell_draw(keys[8], (SEQUENCE_TOTAL, CACHE_POSITIONS, KV_HEADS * HEAD_DIM), 1.0, 6.0, ((0, 16), (2, 2)))
    cache_gates = draw_cache_gates(jax.random.fold_in(keys[20], 71), 0)
    lengths = draw_lengths(jax.random.fold_in(keys[20], 71), 0)
    ffn_gain = jnp.clip(1.0 + 0.18 * jax.random.normal(keys[11], (D,), jnp.float32), 0.099609375, 1.8984375).astype(jnp.bfloat16)
    router_w = bell_draw(keys[12], (D, EXPERTS), D ** -0.5, 0.125)
    routes_keys = jax.random.split(jax.random.fold_in(keys[13], 1), SEQUENCE_TOTAL // SEQ_DEV)
    routes_turns = jax.random.permutation(jax.random.fold_in(keys[13], 3), SEQUENCE_TOTAL // SEQ_DEV)
    routes = jax.vmap(lambda own, number: assign_block(jax.random.fold_in(keys[13], 2), own, number, SEQ_DEV, EXPERTS, TOP_K, CAP, 2))(routes_keys, routes_turns).reshape((SEQUENCE_TOTAL, TOP_K))
    shared_gate = bell_draw(keys[14], (D, SHARED_FF), D ** -0.5, 0.125, ((1, 2),))
    shared_up = bell_draw(keys[15], (D, SHARED_FF), D ** -0.5, 0.125, ((1, 2),))
    shared_down = bell_draw(keys[16], (SHARED_FF, D), SHARED_FF ** -0.5, 0.25, ((0, 2),))
    expert_gate = bell_draw(keys[17], (EXPERTS, D, EXPERT_FF), D ** -0.5, 0.125, ((0, 16), (2, 2)))
    expert_up = bell_draw(keys[18], (EXPERTS, D, EXPERT_FF), D ** -0.5, 0.125, ((0, 16), (2, 2)))
    expert_down = bell_draw(keys[19], (EXPERTS, EXPERT_FF, D), EXPERT_FF ** -0.5, 0.25, ((0, 16), (1, 2)))
    return {"tokens": tokens, "norm_gain": norm_gain, "w_query": w_query, "w_key": w_key, "w_value": w_value, "w_forget": w_forget, "w_out": w_out, "cache_keys": cache_keys, "cache_values": cache_values, "cache_gates": cache_gates, "lengths": lengths, "ffn_gain": ffn_gain, "router_w": router_w, "routes": routes, "shared_gate": shared_gate, "shared_up": shared_up, "shared_down": shared_down, "expert_gate": expert_gate, "expert_up": expert_up, "expert_down": expert_down}


EPS = 1e-06
ROUTE_SCALE = 2.5

def norm_rows(rows, norm_gain):
    values = rows.astype(jnp.float32)
    factor = lax.rsqrt(lax.optimization_barrier(jnp.mean(values * values, axis=-1, keepdims=True)) + EPS)
    return (values * factor * norm_gain.astype(jnp.float32)).astype(jnp.bfloat16)

def parts_sum(left, right, pieces):
    width = left.shape[1] // pieces
    total_rows = jnp.zeros((left.shape[0], right.shape[1]), jnp.float32)
    for piece in range(pieces):
        partial_value = jnp.dot(left[:, piece * width:(piece + 1) * width], right[piece * width:(piece + 1) * width], preferred_element_type=jnp.float32)
        rounded = lax.optimization_barrier(partial_value.astype(jnp.bfloat16))
        total_rows = total_rows + rounded.astype(jnp.float32)
    return total_rows

def swiglu_hidden(rows, w_gate, w_up):
    gate_proj = jnp.dot(rows, w_gate, preferred_element_type=jnp.float32)
    upward = jnp.dot(rows, w_up, preferred_element_type=jnp.float32)
    return (jax.nn.silu(gate_proj) * upward).astype(jnp.bfloat16)

def route_weights(rows, router_w, chosen):
    scores = jax.nn.sigmoid(jnp.dot(rows, router_w, preferred_element_type=jnp.float32))
    picked = jnp.take_along_axis(scores, chosen, axis=1)
    return ROUTE_SCALE * picked / lax.optimization_barrier(jnp.sum(picked, axis=1, keepdims=True))

def attend_rows(inputs):
    queries, key_new, value_new, log_gate, cached_keys, cached_values, cache_gates, lengths = inputs
    seq_count = queries.shape[0]
    group_size = QUERY_HEADS // KV_HEADS
    score_scale = HEAD_DIM ** (-0.5)
    queries = queries.reshape(seq_count, KV_HEADS, group_size, HEAD_DIM).astype(jnp.float32)
    key_new = key_new.reshape(seq_count, KV_HEADS, HEAD_DIM).astype(jnp.float32)
    value_new = value_new.reshape(seq_count, KV_HEADS, HEAD_DIM).astype(jnp.float32)
    cached_keys = cached_keys.reshape(seq_count, CACHE_POSITIONS, KV_HEADS, HEAD_DIM).astype(jnp.float32)
    cached_values = cached_values.reshape(seq_count, CACHE_POSITIONS, KV_HEADS, HEAD_DIM).astype(jnp.float32)
    past_score = jnp.einsum('skgd,slkd->skgl', queries, cached_keys) * score_scale
    last_index = jnp.broadcast_to((lengths - 1).astype(jnp.int32)[:, None, None], (seq_count, QUERY_HEADS, 1))
    last_gate = jnp.take_along_axis(cache_gates, last_index, axis=2)
    gate_bias = last_gate + log_gate[:, :, None] - cache_gates
    past_score = past_score + gate_bias.reshape(seq_count, KV_HEADS, group_size, CACHE_POSITIONS)
    is_valid = jnp.arange(CACHE_POSITIONS)[None, :] < lengths[:, None]
    past_score = jnp.where(is_valid[:, None, None, :], past_score, -jnp.inf)
    self_score = jnp.einsum('skgd,skd->skg', queries, key_new) * score_scale
    peak_score = jnp.maximum(lax.optimization_barrier(jnp.max(past_score, axis=-1)), self_score)
    past_weight = jnp.exp(past_score - peak_score[..., None])
    self_weight = jnp.exp(self_score - peak_score)
    weight_sum = lax.optimization_barrier(jnp.sum(past_weight, axis=-1)) + self_weight
    past_prob = (past_weight / weight_sum[..., None]).astype(jnp.bfloat16).astype(jnp.float32)
    self_prob = (self_weight / weight_sum).astype(jnp.bfloat16).astype(jnp.float32)
    mixed_heads = jnp.einsum('skgl,slkd->skgd', past_prob, cached_values)
    mixed_heads = mixed_heads + self_prob[..., None] * value_new[:, :, None, :]
    return mixed_heads.astype(jnp.bfloat16).reshape(seq_count, QUERY_HEADS * HEAD_DIM)

def reference(tokens, norm_gain, w_query, w_key, w_value, w_forget, w_out, cache_keys, cache_values, cache_gates, lengths, ffn_gain, router_w, routes, shared_gate, shared_up, shared_down, expert_gate, expert_up, expert_down):
    normed = norm_rows(tokens, norm_gain)
    queries = jnp.dot(normed, w_query, preferred_element_type=jnp.float32).astype(jnp.bfloat16)
    keys_new = jnp.dot(normed, w_key, preferred_element_type=jnp.float32).astype(jnp.bfloat16)
    values_new = jnp.dot(normed, w_value, preferred_element_type=jnp.float32).astype(jnp.bfloat16)
    log_gate = jax.nn.log_sigmoid(jnp.dot(normed, w_forget, preferred_element_type=jnp.float32))

    def blocked(array):
        return array.reshape((N_EP, SEQ_DEV) + array.shape[1:])
    attn = lax.map(attend_rows, (blocked(queries), blocked(keys_new), blocked(values_new), blocked(log_gate), blocked(cache_keys), blocked(cache_values), blocked(cache_gates), blocked(lengths)))
    attn = attn.reshape(SEQUENCE_TOTAL, QUERY_HEADS * HEAD_DIM)
    attended = parts_sum(attn, w_out, N_TP)
    residual_rows = (tokens.astype(jnp.float32) + attended).astype(jnp.bfloat16)
    ffn_rows = norm_rows(residual_rows, ffn_gain)
    shared = parts_sum(swiglu_hidden(ffn_rows, shared_gate, shared_up), shared_down, N_TP)
    weights = route_weights(ffn_rows, router_w, routes)
    slot_count = N_EP * CAP

    def add_expert(total_rows, expert_item):
        expert_id, w_gate, w_up, w_down = expert_item
        is_routed = routes == expert_id
        chosen = jnp.any(is_routed, axis=1)
        row_index = jnp.nonzero(chosen, size=slot_count, fill_value=0)[0].astype(jnp.int32)
        live_slot = (jnp.arange(slot_count) < jnp.sum(chosen.astype(jnp.int32))).astype(jnp.float32)
        picked_rows = ffn_rows[row_index]
        answer = parts_sum(swiglu_hidden(picked_rows, w_gate, w_up), w_down, N_TP).astype(jnp.bfloat16)
        route_share = lax.optimization_barrier(jnp.sum(jnp.where(is_routed, weights, 0.0), axis=1))[row_index] * live_slot
        return (total_rows.at[row_index].add(answer.astype(jnp.float32) * route_share[:, None]), None)
    routed, _ = lax.scan(add_expert, jnp.zeros((SEQUENCE_TOTAL, D), jnp.float32), (jnp.arange(EXPERTS, dtype=jnp.int32), expert_gate, expert_up, expert_down))
    return (residual_rows.astype(jnp.float32) + shared + routed).astype(jnp.bfloat16)
```

```python
import functools

import jax
import jax.numpy as jnp
from jax import lax
from jax.experimental import pallas as pl
from jax.experimental.pallas import tpu as pltpu
from jax.sharding import PartitionSpec as P

HEAD_DIM = 64
EPS = 1e-06
ROUTE_SCALE = 2.5
MESH = pl.DeviceIdType.MESH
F32 = jnp.float32
BF16 = jnp.bfloat16


def dot(a, b):
    return jnp.dot(a, b, preferred_element_type=F32)


def dot_t(a, b):
    return lax.dot_general(a, b, (((1,), (1,)), ((), ())), preferred_element_type=F32)


def norm_rows(values, gain):
    factor = lax.rsqrt(jnp.mean(values * values, axis=-1, keepdims=True) + EPS)
    return (values * factor * gain.astype(F32)).astype(BF16)


def silu(x):
    return x * jax.nn.sigmoid(x)


def attend_kernel(
    len_ref, tok_ref, gain_ref, wq_ref, wk_ref, wv_ref, wf_ref, wo_ref, kc_ref, vc_ref, cg_ref,
    out_ref, qs, lg, ss, vn, ob,
):
    step = pl.program_id(0)
    steps = pl.num_programs(0)
    per_step, positions, kv_width = kc_ref.shape
    seqs = tok_ref.shape[0]
    heads = wf_ref.shape[0]
    kv_count = kv_width // HEAD_DIM
    group = heads // kv_count
    scale = HEAD_DIM ** (-0.5)

    @pl.when(step == 0)
    def _():
        normed = norm_rows(tok_ref[...].astype(F32), gain_ref[...])
        q = dot(normed, wq_ref[...]).astype(BF16).astype(F32)
        kn = dot(normed, wk_ref[...]).astype(BF16).astype(F32)
        vn[...] = dot(normed, wv_ref[...]).astype(BF16).astype(F32)
        fg = dot_t(normed, wf_ref[...])
        log_gate = jnp.minimum(fg, 0.0) - jnp.log1p(jnp.exp(-jnp.abs(fg)))
        lane = lax.broadcasted_iota(jnp.int32, (seqs, kv_width), 1)
        for h in range(heads):
            kv = h // group
            base = (h * HEAD_DIM) // kv_width * kv_width
            blk = q[:, base : base + kv_width]
            shift = (kv * HEAD_DIM - (h * HEAD_DIM - base)) % kv_width
            if shift:
                blk = pltpu.roll(blk, shift, 1)
            blk = jnp.where((lane >= kv * HEAD_DIM) & (lane < (kv + 1) * HEAD_DIM), blk, 0.0)
            qs[:, h, :] = blk
            lg[:, h, :] = jnp.broadcast_to(log_gate[:, h : h + 1], (seqs, 128))
            own = jnp.sum(blk * kn, axis=1, keepdims=True) * scale
            ss[:, h, :] = jnp.broadcast_to(own, (seqs, 128))

    pos = lax.broadcasted_iota(jnp.int32, (heads, positions), 1)
    lane1 = lax.broadcasted_iota(jnp.int32, (1, kv_width), 1)
    for j in range(per_step):
        b = step * per_step + j
        n = len_ref[b]
        score = dot_t(qs[b].astype(BF16), kc_ref[j])
        gates = cg_ref[j]
        last = jnp.sum(jnp.where(pos == n - 1, gates, 0.0), axis=1, keepdims=True)
        score = score * scale + (last + lg[b][:, :1] - gates)
        score = jnp.where(pos < n, score, -jnp.inf)
        own = ss[b][:, :1]
        peak = jnp.maximum(jnp.max(score, axis=1, keepdims=True), own)
        weight = jnp.exp(score - peak)
        own_weight = jnp.exp(own - peak)
        inv = 1.0 / (jnp.sum(weight, axis=1, keepdims=True) + own_weight)
        prob = (weight * inv).astype(BF16)
        own_prob = (own_weight * inv).astype(BF16).astype(F32)
        mixed = dot(prob, vc_ref[j]) + own_prob * vn[pl.ds(b, 1), :]
        for g in range(group):
            row = mixed[g : g + 1]
            for kv in range(1, kv_count):
                row = jnp.where(lane1 >= kv * HEAD_DIM, mixed[kv * group + g : kv * group + g + 1], row)
            ob[g, pl.ds(b, 1), :] = row

    @pl.when(step == steps - 1)
    def _():
        total = jnp.zeros((seqs, wo_ref.shape[1]), F32)
        for g in range(group):
            rows = [
                wo_ref[(kv * group + g) * HEAD_DIM : (kv * group + g + 1) * HEAD_DIM, :]
                for kv in range(kv_count)
            ]
            total = total + dot(ob[g].astype(BF16), jnp.concatenate(rows, axis=0))
        out_ref[...] = total.astype(BF16)


def experts_kernel(
    n, per_chunk, part_ref, tok_ref, gain_ref, router_ref, routes_ref,
    sg_hbm, su_hbm, sd_hbm, eg_hbm, eu_hbm, ed_hbm, out_ref,
    sg, su, sd, eg, eu, ed, other, rows_all, resid, sh_send, sh_recv, sh_keep,
    p_send, p_recv, p_keep, answer, ret, halves, weights,
    wsem, tsend, trecv, dsend, drecv, rsend, rrecv, psend, precv, asend, arecv,
):
    i = lax.axis_index("ep")
    t = lax.axis_index("tp")
    u = 1 - t
    seqs, width = tok_ref.shape
    half = width // 2
    chunks = n // per_chunk
    rows = per_chunk * seqs
    partner = (i, u)

    loads = [
        pltpu.make_async_copy(sg_hbm, sg, wsem.at[0]),
        pltpu.make_async_copy(su_hbm, su, wsem.at[1]),
        pltpu.make_async_copy(sd_hbm.at[:, pl.ds(0, half)], sd.at[0], wsem.at[2]),
        pltpu.make_async_copy(sd_hbm.at[:, pl.ds(half, half)], sd.at[1], wsem.at[3]),
        pltpu.make_async_copy(eg_hbm.at[0], eg, wsem.at[4]),
        pltpu.make_async_copy(eu_hbm.at[0], eu, wsem.at[5]),
        pltpu.make_async_copy(ed_hbm.at[0, :, pl.ds(0, half)], ed.at[0], wsem.at[6]),
        pltpu.make_async_copy(ed_hbm.at[0, :, pl.ds(half, half)], ed.at[1], wsem.at[7]),
    ]
    for load in loads:
        load.start()

    barrier = pltpu.get_barrier_semaphore()
    pl.semaphore_signal(barrier, inc=1, device_id=partner, device_id_type=MESH)

    @pl.loop(1, n)
    def _(k):
        pl.semaphore_signal(barrier, inc=1, device_id=(lax.rem(i + k, n), t), device_id_type=MESH)

    pl.semaphore_wait(barrier, n)

    def remote(src, dst, ssem, rsem, dev):
        return pltpu.make_async_remote_copy(
            src_ref=src, dst_ref=dst, send_sem=ssem, recv_sem=rsem, device_id=dev,
            device_id_type=MESH,
        )

    swap = remote(part_ref, other, tsend.at[0], trecv.at[0], partner)
    swap.start()
    swap.wait()
    attended = part_ref[...].astype(F32) + other[...].astype(F32)
    residual = (tok_ref[...].astype(F32) + attended).astype(BF16)
    ffn = norm_rows(residual.astype(F32), gain_ref[...])
    for s in range(2):
        rows_all[s, i] = ffn[:, s * half : (s + 1) * half]
        resid[s] = residual[:, s * half : (s + 1) * half]

    def gather_copy(slot, dev):
        return remote(
            rows_all.at[t, slot], rows_all.at[t, slot], dsend.at[dev], drecv.at[slot], (dev, t)
        )

    @pl.loop(1, n)
    def _(k):
        gather_copy(i, lax.rem(i + k, n)).start()

    for load in loads[:4]:
        load.wait()
    hidden = (silu(dot(ffn, sg[...])) * dot(ffn, su[...])).astype(BF16)
    sh_send[...] = dot(hidden, sd[u]).astype(BF16)
    shared_swap = remote(sh_send, sh_recv, tsend.at[1], trecv.at[1], partner)
    shared_swap.start()
    sh_keep[...] = dot(hidden, sd[t]).astype(BF16)
    scores = jax.nn.sigmoid(dot_t(router_ref[...], ffn))
    expert_id = lax.broadcasted_iota(jnp.int32, scores.shape, 0)
    routes = routes_ref[...]
    named = routes[0:1] == expert_id
    for k in range(1, routes.shape[0]):
        named = named | (routes[k : k + 1] == expert_id)
    picked = jnp.where(named, scores, 0.0)
    weights[...] = ROUTE_SCALE * picked / jnp.sum(picked, axis=0, keepdims=True)
    diagonal = lax.broadcasted_iota(jnp.int32, (seqs, seqs), 0) == lax.broadcasted_iota(
        jnp.int32, (seqs, seqs), 1
    )
    for load in loads[4:]:
        load.wait()

    def relay(slot):
        return remote(
            rows_all.at[t, slot], rows_all.at[t, slot], rsend.at[slot], rrecv.at[slot], partner
        )

    def relay_in(slot):
        return remote(
            rows_all.at[u, slot], rows_all.at[u, slot], rsend.at[slot], rrecv.at[slot], partner
        )

    def chunk_of(c):
        return lax.rem(i // per_chunk + c, chunks)

    def start_relays(c):
        @pl.loop(0, per_chunk)
        def _(m):
            slot = chunk_of(c) * per_chunk + m

            @pl.when(slot != i)
            def _():
                gather_copy(slot, slot).wait_recv()
                relay(slot).start()

    def part_swap(c):
        return remote(p_send.at[c], p_recv.at[c], psend.at[c], precv.at[c], partner)

    def answer_copy(slot):
        return remote(answer.at[slot], ret.at[i], asend.at[slot], arecv.at[i], (slot, t))

    def finish(c):
        part_swap(c).wait_recv()
        total = (p_keep[c].astype(F32) + p_recv[c].astype(F32)).astype(BF16)
        first = chunk_of(c) * per_chunk
        answer[pl.ds(first, per_chunk)] = total.reshape(per_chunk, seqs, half)

        @pl.loop(0, per_chunk)
        def _(m):
            slot = first + m

            @pl.when(slot != i)
            def _():
                answer_copy(slot).start()

    start_relays(0)

    @pl.loop(0, chunks)
    def _(c):
        @pl.when(c + 1 < chunks)
        def _():
            start_relays(c + 1)

        first = chunk_of(c) * per_chunk

        @pl.loop(0, per_chunk)
        def _(m):
            slot = first + m

            @pl.when(slot != i)
            def _():
                relay_in(slot).wait_recv()

        x0 = rows_all[0, pl.ds(first, per_chunk)].reshape(rows, half)
        x1 = rows_all[1, pl.ds(first, per_chunk)].reshape(rows, half)
        gate = dot(x0, eg[:half]) + dot(x1, eg[half:])
        up = dot(x0, eu[:half]) + dot(x1, eu[half:])
        hid = (silu(gate) * up).astype(BF16)
        p_send[c] = dot(hid, ed[u]).astype(BF16)
        part_swap(c).start()
        p_keep[c] = dot(hid, ed[t]).astype(BF16)

        @pl.when(c > 0)
        def _():
            finish(c - 1)

    finish(chunks - 1)
    shared_swap.wait()
    base = resid[t].astype(F32) + (sh_keep[...].astype(F32) + sh_recv[...].astype(F32))

    def weight_of(e):
        return jnp.sum(jnp.where(diagonal, weights[pl.ds(e, 1), :], 0.0), axis=1, keepdims=True)

    routed = weight_of(i) * answer[i].astype(F32)

    def add(k, acc):
        e = lax.rem(i + k, n)
        remote(answer.at[e], ret.at[e], asend.at[e], arecv.at[e], (e, t)).wait_recv()
        return acc + weight_of(e) * ret[e].astype(F32)

    routed = lax.fori_loop(1, n, add, routed)
    halves[t] = (base + routed).astype(BF16)
    last = remote(halves.at[t], halves.at[t], tsend.at[2], trecv.at[2], partner)
    last.start()

    @pl.loop(1, n)
    def _(k):
        e = lax.rem(i + k, n)
        gather_copy(i, e).wait_send()
        relay(e).wait_send()
        answer_copy(e).wait_send()

    @pl.loop(0, chunks)
    def _(c):
        part_swap(c).wait_send()

    last.wait_send()
    remote(halves.at[u], halves.at[u], tsend.at[2], trecv.at[2], partner).wait_recv()
    for s in range(2):
        out_ref[:, s * half : (s + 1) * half] = halves[s]


def per_device(
    tokens, norm_gain, w_query, w_key, w_value, w_forget, w_out, cache_keys, cache_values,
    cache_gates, lengths, ffn_gain, router_w, routes, shared_gate, shared_up, shared_down,
    expert_gate, expert_up, expert_down,
):
    seqs, width = tokens.shape
    half = width // 2
    n = lax.axis_size("ep")
    positions, kv_width = cache_keys.shape[1:]
    heads = w_forget.shape[1]
    group = heads * HEAD_DIM // kv_width
    per_step = 4

    def whole(a):
        return pl.BlockSpec(a.shape, lambda s: (0,) * a.ndim)

    w_forget = w_forget.T
    partial_value = pl.pallas_call(
        attend_kernel,
        grid=(seqs // per_step,),
        in_specs=[pl.BlockSpec(memory_space=pltpu.SMEM)]
        + [whole(a) for a in (tokens, norm_gain, w_query, w_key, w_value, w_forget, w_out)]
        + [
            pl.BlockSpec((per_step, positions, kv_width), lambda s: (s, 0, 0)),
            pl.BlockSpec((per_step, positions, kv_width), lambda s: (s, 0, 0)),
            pl.BlockSpec((per_step, heads, positions), lambda s: (s, 0, 0)),
        ],
        out_specs=pl.BlockSpec((seqs, width), lambda s: (0, 0)),
        out_shape=jax.ShapeDtypeStruct((seqs, width), BF16),
        scratch_shapes=[
            pltpu.VMEM((seqs, heads, kv_width), F32),
            pltpu.VMEM((seqs, heads, 128), F32),
            pltpu.VMEM((seqs, heads, 128), F32),
            pltpu.VMEM((seqs, kv_width), F32),
            pltpu.VMEM((group, seqs, kv_width), F32),
        ],
        compiler_params=pltpu.CompilerParams(
            dimension_semantics=("arbitrary",)
        ),
        name="attend",
    )(lengths, tokens, norm_gain, w_query, w_key, w_value, w_forget, w_out, cache_keys, cache_values,
      cache_gates)

    per_chunk = 4
    chunks = n // per_chunk
    rows = per_chunk * seqs
    ff = shared_gate.shape[1]
    eff = expert_gate.shape[2]
    vmem = pl.BlockSpec(memory_space=pltpu.VMEM)
    hbm = pl.BlockSpec(memory_space=pl.ANY)
    dma = pltpu.SemaphoreType.DMA
    return pl.pallas_call(
        functools.partial(experts_kernel, n, per_chunk),
        in_specs=[vmem] * 5 + [hbm] * 6,
        out_specs=vmem,
        out_shape=jax.ShapeDtypeStruct((seqs, width), BF16),
        scratch_shapes=[
            pltpu.VMEM((width, ff), BF16),
            pltpu.VMEM((width, ff), BF16),
            pltpu.VMEM((2, ff, half), BF16),
            pltpu.VMEM((width, eff), BF16),
            pltpu.VMEM((width, eff), BF16),
            pltpu.VMEM((2, eff, half), BF16),
            pltpu.VMEM((seqs, width), BF16),
            pltpu.VMEM((2, n, seqs, half), BF16),
            pltpu.VMEM((2, seqs, half), BF16),
            pltpu.VMEM((seqs, half), BF16),
            pltpu.VMEM((seqs, half), BF16),
            pltpu.VMEM((seqs, half), BF16),
            pltpu.VMEM((chunks, rows, half), BF16),
            pltpu.VMEM((chunks, rows, half), BF16),
            pltpu.VMEM((chunks, rows, half), BF16),
            pltpu.VMEM((n, seqs, half), BF16),
            pltpu.VMEM((n, seqs, half), BF16),
            pltpu.VMEM((2, seqs, half), BF16),
            pltpu.VMEM((n, seqs), F32),
            dma((8,)), dma((3,)), dma((3,)),
            dma((n,)), dma((n,)), dma((n,)), dma((n,)),
            dma((chunks,)), dma((chunks,)), dma((n,)), dma((n,)),
        ],
        compiler_params=pltpu.CompilerParams(
            collective_id=0, has_side_effects=True
        ),
        name="experts",
    )(partial_value, tokens, ffn_gain, router_w.T, routes.T, shared_gate, shared_up,
      shared_down, expert_gate, expert_up, expert_down)


def solution(mesh):
    placed = (
        P("ep", None),
        P(),
        P(None, "tp"),
        P(None, "tp"),
        P(None, "tp"),
        P(None, "tp"),
        P("tp", None),
        P("ep", None, "tp"),
        P("ep", None, "tp"),
        P("ep", "tp", None),
        P("ep"),
        P(),
        P(),
        P("ep", None),
        P(None, "tp"),
        P(None, "tp"),
        P("tp", None),
        P("ep", None, "tp"),
        P("ep", None, "tp"),
        P("ep", "tp", None),
    )
    return jax.shard_map(
        per_device, mesh=mesh, in_specs=placed, out_specs=P("ep", None), check_vma=False
    )
```

```python
import functools

import jax
import jax.numpy as jnp
from jax import lax
from jax.experimental import pallas as pl
from jax.experimental.pallas import tpu as pltpu
from jax.sharding import PartitionSpec as P

HEAD_DIM = 64
EPS = 1e-06
ROUTE_SCALE = 2.5
MESH = pl.DeviceIdType.MESH
F32 = jnp.float32
BF16 = jnp.bfloat16


def dot(a, b):
    return jnp.dot(a, b, preferred_element_type=F32)


def dot_t(a, b):
    return lax.dot_general(a, b, (((1,), (1,)), ((), ())), preferred_element_type=F32)


def norm_rows(values, gain):
    factor = lax.rsqrt(jnp.mean(values * values, axis=-1, keepdims=True) + EPS)
    return (values * factor * gain.astype(F32)).astype(BF16)


def silu(x):
    return x * jax.nn.sigmoid(x)


def attend_kernel(
    len_ref, tok_ref, gain_ref, wq_ref, wk_ref, wv_ref, wf_ref, wo_ref, kc_ref, vc_ref, cg_ref,
    out_ref, qs, lg, ss, vn, ob,
):
    step = pl.program_id(0)
    steps = pl.num_programs(0)
    per_step, positions, kv_width = kc_ref.shape
    seqs = tok_ref.shape[0]
    heads = wf_ref.shape[0]
    kv_count = kv_width // HEAD_DIM
    group = heads // kv_count
    scale = HEAD_DIM ** (-0.5)

    @pl.when(step == 0)
    def _():
        normed = norm_rows(tok_ref[...].astype(F32), gain_ref[...])
        q = dot(normed, wq_ref[...]).astype(BF16).astype(F32)
        kn = dot(normed, wk_ref[...]).astype(BF16).astype(F32)
        vn[...] = dot(normed, wv_ref[...]).astype(BF16).astype(F32)
        fg = dot_t(normed, wf_ref[...])
        log_gate = jnp.minimum(fg, 0.0) - jnp.log1p(jnp.exp(-jnp.abs(fg)))
        lane = lax.broadcasted_iota(jnp.int32, (seqs, kv_width), 1)
        for h in range(heads):
            kv = h // group
            base = (h * HEAD_DIM) // kv_width * kv_width
            blk = q[:, base : base + kv_width]
            shift = (kv * HEAD_DIM - (h * HEAD_DIM - base)) % kv_width
            if shift:
                blk = pltpu.roll(blk, shift, 1)
            blk = jnp.where((lane >= kv * HEAD_DIM) & (lane < (kv + 1) * HEAD_DIM), blk, 0.0)
            qs[:, h, :] = blk
            lg[:, h, :] = jnp.broadcast_to(log_gate[:, h : h + 1], (seqs, 128))
            own = jnp.sum(blk * kn, axis=1, keepdims=True) * scale
            ss[:, h, :] = jnp.broadcast_to(own, (seqs, 128))

    pos = lax.broadcasted_iota(jnp.int32, (heads, positions), 1)
    lane1 = lax.broadcasted_iota(jnp.int32, (1, kv_width), 1)
    for j in range(per_step):
        b = step * per_step + j
        n = len_ref[b]
        score = dot_t(qs[b].astype(BF16), kc_ref[j])
        gates = cg_ref[j]
        last = jnp.sum(jnp.where(pos == n - 1, gates, 0.0), axis=1, keepdims=True)
        score = score * scale + (last + lg[b][:, :1] - gates)
        score = jnp.where(pos < n, score, -jnp.inf)
        own = ss[b][:, :1]
        peak = jnp.maximum(jnp.max(score, axis=1, keepdims=True), own)
        weight = jnp.exp(score - peak)
        own_weight = jnp.exp(own - peak)
        inv = 1.0 / (jnp.sum(weight, axis=1, keepdims=True) + own_weight)
        prob = (weight * inv).astype(BF16)
        own_prob = (own_weight * inv).astype(BF16).astype(F32)
        mixed = dot(prob, vc_ref[j]) + own_prob * vn[pl.ds(b, 1), :]
        for g in range(group):
            row = mixed[g : g + 1]
            for kv in range(1, kv_count):
                row = jnp.where(lane1 >= kv * HEAD_DIM, mixed[kv * group + g : kv * group + g + 1], row)
            ob[g, pl.ds(b, 1), :] = row

    @pl.when(step == steps - 1)
    def _():
        total = jnp.zeros((seqs, wo_ref.shape[1]), F32)
        for g in range(group):
            rows = [
                wo_ref[(kv * group + g) * HEAD_DIM : (kv * group + g + 1) * HEAD_DIM, :]
                for kv in range(kv_count)
            ]
            total = total + dot(ob[g].astype(BF16), jnp.concatenate(rows, axis=0))
        out_ref[...] = total.astype(BF16)


def experts_kernel(
    n, q, part_ref, tok_ref, gain_ref, router_ref, routes_ref,
    sg_hbm, su_hbm, sd_hbm, eg_hbm, eu_hbm, ed_hbm, out_ref,
    sg, su, sd, eg, eu, ed, other, rows_all, resid, sh_send, sh_recv, sh_keep,
    p_send, p_recv, p_keep, answer, mid, out_sums, in_sums, halves, weights,
    wsem, tsend, trecv, csend, psend, drecv, rsend, rrecv, xsend, xrecv, asend, arecv,
    fsend, frecv, vsend, vrecv,
):
    i = lax.axis_index("ep")
    t = lax.axis_index("tp")
    u = 1 - t
    seqs, width = tok_ref.shape
    half = width // 2
    planes = n // q
    rows = q * seqs
    partner = (i, u)
    zi = i // q
    pi = lax.rem(i, q)

    loads = [
        pltpu.make_async_copy(sg_hbm, sg, wsem.at[0]),
        pltpu.make_async_copy(su_hbm, su, wsem.at[1]),
        pltpu.make_async_copy(sd_hbm.at[:, pl.ds(0, half)], sd.at[0], wsem.at[2]),
        pltpu.make_async_copy(sd_hbm.at[:, pl.ds(half, half)], sd.at[1], wsem.at[3]),
        pltpu.make_async_copy(eg_hbm.at[0], eg, wsem.at[4]),
        pltpu.make_async_copy(eu_hbm.at[0], eu, wsem.at[5]),
        pltpu.make_async_copy(ed_hbm.at[0, :, pl.ds(0, half)], ed.at[0], wsem.at[6]),
        pltpu.make_async_copy(ed_hbm.at[0, :, pl.ds(half, half)], ed.at[1], wsem.at[7]),
    ]
    for load in loads:
        load.start()

    def plane_of(c):
        return lax.rem(zi + c, planes)

    def place_of(k):
        return lax.rem(pi + k, q)

    barrier = pltpu.get_barrier_semaphore()
    pl.semaphore_signal(barrier, inc=1, device_id=partner, device_id_type=MESH)
    for c in range(1, planes):
        pl.semaphore_signal(
            barrier, inc=1, device_id=(plane_of(c) * q + pi, t), device_id_type=MESH
        )
    for k in range(1, q):
        pl.semaphore_signal(
            barrier, inc=1, device_id=(zi * q + place_of(k), t), device_id_type=MESH
        )
    pl.semaphore_wait(barrier, planes + q - 1)

    def remote(src, dst, ssem, rsem, dev):
        return pltpu.make_async_remote_copy(
            src_ref=src, dst_ref=dst, send_sem=ssem, recv_sem=rsem, device_id=dev,
            device_id_type=MESH,
        )

    swap = remote(part_ref, other, tsend.at[0], trecv.at[0], partner)
    swap.start()
    swap.wait()
    attended = part_ref[...].astype(F32) + other[...].astype(F32)
    residual = (tok_ref[...].astype(F32) + attended).astype(BF16)
    ffn = norm_rows(residual.astype(F32), gain_ref[...])
    for s in range(2):
        rows_all[s, i] = ffn[:, s * half : (s + 1) * half]
        resid[s] = residual[:, s * half : (s + 1) * half]

    def landed(dst, rsem):
        remote(dst, dst, rsend.at[0], rsem, partner).wait_recv()

    def gathered(slot, ssem, dev):
        return remote(rows_all.at[t, slot], rows_all.at[t, slot], ssem, drecv.at[slot], dev)

    def column_copy(slot, plane):
        return gathered(slot, csend.at[plane], (plane * q + pi, t))

    def plane_copy(slot, place):
        return gathered(slot, psend.at[slot // q * q + place], (zi * q + place, t))

    def relay(slot):
        return remote(
            rows_all.at[t, slot], rows_all.at[t, slot], rsend.at[slot], rrecv.at[slot], partner
        )

    def relay_in(slot):
        landed(rows_all.at[u, slot], rrecv.at[slot])

    def spread(slot):
        for k in range(1, q):
            plane_copy(slot, place_of(k)).start()

    for c in range(1, planes):
        column_copy(i, plane_of(c)).start()
    spread(i)

    scores = jax.nn.sigmoid(dot_t(router_ref[...], ffn))
    expert_id = lax.broadcasted_iota(jnp.int32, scores.shape, 0)
    routes = routes_ref[...]
    named = routes[0:1] == expert_id
    for k in range(1, routes.shape[0]):
        named = named | (routes[k : k + 1] == expert_id)
    picked = jnp.where(named, scores, 0.0)
    weights[zi] = jnp.zeros(weights.shape[1:], F32)
    weights[zi, :, 0:seqs] = ROUTE_SCALE * picked / jnp.sum(picked, axis=0, keepdims=True)
    diagonal = lax.broadcasted_iota(jnp.int32, (seqs, seqs), 0) == lax.broadcasted_iota(
        jnp.int32, (seqs, seqs), 1
    )

    def weight_copy(src, plane):
        return remote(
            weights.at[src], weights.at[src], vsend.at[plane], vrecv.at[src], (plane * q + pi, t)
        )

    for c in range(1, planes):
        weight_copy(zi, plane_of(c)).start()

    for load in loads[:4]:
        load.wait()
    hidden = (silu(dot(ffn, sg[...])) * dot(ffn, su[...])).astype(BF16)
    sh_send[...] = dot(hidden, sd[u]).astype(BF16)
    shared_swap = remote(sh_send, sh_recv, tsend.at[1], trecv.at[1], partner)
    shared_swap.start()

    def pass_on(c):
        slot = plane_of(c) * q + pi
        landed(rows_all.at[t, slot], drecv.at[slot])
        spread(slot)
        relay(slot).start()

    for c in range(1, planes):
        pass_on(c)
    sh_keep[...] = dot(hidden, sd[t]).astype(BF16)
    for load in loads[4:]:
        load.wait()

    def start_relays(c):
        for k in range(1, q):
            slot = plane_of(c) * q + place_of(k)
            landed(rows_all.at[t, slot], drecv.at[slot])
            relay(slot).start()

    def part_swap(c):
        return remote(p_send.at[c], p_recv.at[c], xsend.at[c], xrecv.at[c], partner)

    def answer_copy(plane, src, place):
        return remote(
            answer.at[plane * q + place], mid.at[plane * q + src], asend.at[plane * q + place],
            arecv.at[plane * q + src], (zi * q + place, t),
        )

    def sum_copy(src, plane):
        return remote(
            out_sums.at[plane], in_sums.at[src], fsend.at[plane], frecv.at[src], (plane * q + pi, t)
        )

    def compute(c):
        first = plane_of(c) * q
        for k in range(1 if isinstance(c, int) and c == 0 else 0, q):
            relay_in(first + place_of(k))
        x0 = rows_all[0, pl.ds(first, q)].reshape(rows, half)
        x1 = rows_all[1, pl.ds(first, q)].reshape(rows, half)
        gate = dot(x0, eg[:half]) + dot(x1, eg[half:])
        up = dot(x0, eu[:half]) + dot(x1, eu[half:])
        hid = (silu(gate) * up).astype(BF16)
        p_send[c] = dot(hid, ed[u]).astype(BF16)
        part_swap(c).start()
        p_keep[c] = dot(hid, ed[t]).astype(BF16)

    def finish(c):
        part_swap(c).wait_recv()
        total = (p_keep[c].astype(F32) + p_recv[c].astype(F32)).astype(BF16)
        plane = plane_of(c)
        answer[pl.ds(plane * q, q)] = total.reshape(q, seqs, half)
        for k in range(1, q):
            answer_copy(plane, pi, place_of(k)).start()

    def plane_sum(c):
        plane = plane_of(c)
        if not (isinstance(c, int) and c == 0):
            landed(weights.at[plane], vrecv.at[plane])
        total = jnp.zeros((seqs, half), F32)
        for k in range(q):
            place = place_of(k)
            if k:
                landed(mid.at[plane * q + place], arecv.at[plane * q + place])
                block = mid[plane * q + place]
            else:
                block = answer[plane * q + pi]
            row = weights[plane, pl.ds(zi * q + place, 1), 0:seqs]
            column = jnp.sum(jnp.where(diagonal, row, 0.0), axis=1, keepdims=True)
            total = total + column * block.astype(F32)
        if isinstance(c, int) and c == 0:
            return total
        out_sums[plane] = total.astype(BF16)
        sum_copy(zi, plane).start()

    start_relays(0)
    if planes > 1:
        start_relays(1)
    compute(0)

    @pl.loop(1, planes)
    def _(c):
        @pl.when(c + 1 < planes)
        def _():
            start_relays(c + 1)

        compute(c)
        finish(c - 1)

        @pl.when(c > 2)
        def _():
            plane_sum(c - 2)

    finish(planes - 1)
    shared_swap.wait()
    routed = plane_sum(0)
    for c in range(max(1, planes - 2), planes):
        plane_sum(c)
    routed = routed + (
        resid[t].astype(F32) + (sh_keep[...].astype(F32) + sh_recv[...].astype(F32))
    )
    for c in range(1, planes):
        plane = plane_of(c)
        landed(in_sums.at[plane], frecv.at[plane])
        routed = routed + in_sums[plane].astype(F32)
    halves[t] = routed.astype(BF16)
    last = remote(halves.at[t], halves.at[t], tsend.at[2], trecv.at[2], partner)
    last.start()

    for c in range(planes):
        plane = plane_of(c)
        part_swap(c).wait_send()
        if c:
            column_copy(i, plane).wait_send()
            weight_copy(zi, plane).wait_send()
            sum_copy(zi, plane).wait_send()
        for k in range(q):
            if k:
                plane_copy(plane * q + pi, place_of(k)).wait_send()
                answer_copy(plane, pi, place_of(k)).wait_send()
            if c or k:
                relay(plane * q + place_of(k)).wait_send()

    last.wait_send()
    landed(halves.at[u], trecv.at[2])
    for s in range(2):
        out_ref[:, s * half : (s + 1) * half] = halves[s]


def per_device(
    tokens, norm_gain, w_query, w_key, w_value, w_forget, w_out, cache_keys, cache_values,
    cache_gates, lengths, ffn_gain, router_w, routes, shared_gate, shared_up, shared_down,
    expert_gate, expert_up, expert_down,
):
    seqs, width = tokens.shape
    half = width // 2
    n = lax.axis_size("ep")
    positions, kv_width = cache_keys.shape[1:]
    heads = w_forget.shape[1]
    group = heads * HEAD_DIM // kv_width
    per_step = 4

    def whole(a):
        return pl.BlockSpec(a.shape, lambda s: (0,) * a.ndim)

    w_forget = w_forget.T
    partial_value = pl.pallas_call(
        attend_kernel,
        grid=(seqs // per_step,),
        in_specs=[pl.BlockSpec(memory_space=pltpu.SMEM)]
        + [whole(a) for a in (tokens, norm_gain, w_query, w_key, w_value, w_forget, w_out)]
        + [
            pl.BlockSpec((per_step, positions, kv_width), lambda s: (s, 0, 0)),
            pl.BlockSpec((per_step, positions, kv_width), lambda s: (s, 0, 0)),
            pl.BlockSpec((per_step, heads, positions), lambda s: (s, 0, 0)),
        ],
        out_specs=pl.BlockSpec((seqs, width), lambda s: (0, 0)),
        out_shape=jax.ShapeDtypeStruct((seqs, width), BF16),
        scratch_shapes=[
            pltpu.VMEM((seqs, heads, kv_width), F32),
            pltpu.VMEM((seqs, heads, 128), F32),
            pltpu.VMEM((seqs, heads, 128), F32),
            pltpu.VMEM((seqs, kv_width), F32),
            pltpu.VMEM((group, seqs, kv_width), F32),
        ],
        compiler_params=pltpu.CompilerParams(
            dimension_semantics=("arbitrary",)
        ),
        name="attend",
    )(lengths, tokens, norm_gain, w_query, w_key, w_value, w_forget, w_out, cache_keys, cache_values,
      cache_gates)

    per_chunk = 4
    chunks = n // per_chunk
    rows = per_chunk * seqs
    ff = shared_gate.shape[1]
    eff = expert_gate.shape[2]
    vmem = pl.BlockSpec(memory_space=pltpu.VMEM)
    hbm = pl.BlockSpec(memory_space=pl.ANY)
    dma = pltpu.SemaphoreType.DMA
    return pl.pallas_call(
        functools.partial(experts_kernel, n, per_chunk),
        in_specs=[vmem] * 5 + [hbm] * 6,
        out_specs=vmem,
        out_shape=jax.ShapeDtypeStruct((seqs, width), BF16),
        scratch_shapes=[
            pltpu.VMEM((width, ff), BF16),
            pltpu.VMEM((width, ff), BF16),
            pltpu.VMEM((2, ff, half), BF16),
            pltpu.VMEM((width, eff), BF16),
            pltpu.VMEM((width, eff), BF16),
            pltpu.VMEM((2, eff, half), BF16),
            pltpu.VMEM((seqs, width), BF16),
            pltpu.VMEM((2, n, seqs, half), BF16),
            pltpu.VMEM((2, seqs, half), BF16),
            pltpu.VMEM((seqs, half), BF16),
            pltpu.VMEM((seqs, half), BF16),
            pltpu.VMEM((seqs, half), BF16),
            pltpu.VMEM((chunks, rows, half), BF16),
            pltpu.VMEM((chunks, rows, half), BF16),
            pltpu.VMEM((chunks, rows, half), BF16),
            pltpu.VMEM((n, seqs, half), BF16),
            pltpu.VMEM((n, seqs, half), BF16),
            pltpu.VMEM((chunks, seqs, half), BF16),
            pltpu.VMEM((chunks, seqs, half), BF16),
            pltpu.VMEM((2, seqs, half), BF16),
            pltpu.VMEM((chunks, n, 128), F32),
            dma((8,)), dma((3,)), dma((3,)),
            dma((chunks,)), dma((n,)), dma((n,)), dma((n,)), dma((n,)),
            dma((chunks,)), dma((chunks,)), dma((n,)), dma((n,)),
            dma((chunks,)), dma((chunks,)), dma((chunks,)), dma((chunks,)),
        ],
        compiler_params=pltpu.CompilerParams(
            collective_id=0, has_side_effects=True
        ),
        name="experts",
    )(partial_value, tokens, ffn_gain, router_w.T, routes.T, shared_gate, shared_up,
      shared_down, expert_gate, expert_up, expert_down)


def solution(mesh):
    placed = (
        P("ep", None),
        P(),
        P(None, "tp"),
        P(None, "tp"),
        P(None, "tp"),
        P(None, "tp"),
        P("tp", None),
        P("ep", None, "tp"),
        P("ep", None, "tp"),
        P("ep", "tp", None),
        P("ep"),
        P(),
        P(),
        P("ep", None),
        P(None, "tp"),
        P(None, "tp"),
        P("tp", None),
        P("ep", None, "tp"),
        P("ep", None, "tp"),
        P("ep", "tp", None),
    )
    return jax.shard_map(
        per_device, mesh=mesh, in_specs=placed, out_specs=P("ep", None), check_vma=False
    )
```
